1024 devices in a mesh: sp: 256 (over z, y, core), tp: 4 (over x).
Axes of the slice: x: 4, y: 8, z: 16, core: 2. Of those that a mesh axis runs over, the one named last changes fastest.
Arguments:
- query_rows: bfloat16 [163840, 1536], P('sp', 'tp'), may hold values from -8 to 8
- key_rows: bfloat16 [163840, 1536], P('sp', 'tp'), may hold values from -8 to 8
- value_rows: bfloat16 [163840, 1536], P('sp', 'tp'), may hold values from -6 to 6
- query_gain: bfloat16 [64], replicated, may hold values from 0.25 to 4.2
- key_gain: bfloat16 [64], replicated, may hold values from 0.25 to 4.2
- position_bias: bfloat16 [24, 320], P('tp'), may hold values from -165 to 3
- output_grad: bfloat16 [163840, 1536], P('sp', 'tp'), may hold values from -24 to 24
Outputs:
- query_grad: bfloat16 [163840, 1536], P('sp', 'tp')
- key_grad: bfloat16 [163840, 1536], P('sp', 'tp')
- value_grad: bfloat16 [163840, 1536], P('sp', 'tp')
- bias_grad: float32 [24, 320], P('tp')
- query_gain_grad: float32 [64], replicated
- key_gain_grad: float32 [64], replicated
The draws below stay inside these ranges and needn't reach their ends.
All inputs are finite; a program needn't handle non-finite values.
Results may differ from the reference program's by a relative error of at most 0.0055.
The reference program's roundings to bfloat16 on the way count: a program that leaves them out, or rounds other values in their place, can miss the bound.
Values may be sent and summed in bfloat16 or wider, within the bound.
No kernel may reach another device: no remote copies, remote signals or barrier semaphores. Data moves between devices by JAX's collectives and lax.ppermute only.
A program may use at most 128 MiB of HBM per device.

```python
import jax
import jax.numpy as jnp
import numpy as np
from jax import lax

HEADS = 24
HEAD_DIM = 64
SEG = 64
LEFT = 8
CLIP = 256
TOK_DEV = 640
SEQ = 163840


def planted_pair(base):
    key_part = jax.random.normal(jax.random.fold_in(base, 101), (SEQ, HEADS * HEAD_DIM), jnp.float32)
    query_part = jax.random.normal(jax.random.fold_in(base, 202), (SEQ, HEADS * HEAD_DIM), jnp.float32)
    return (jnp.clip(query_part, -8.0, 8.0), jnp.clip(key_part, -8.0, 8.0))


def draw_query_rows(key, part):
    return planted_pair(key)[0].astype(jnp.bfloat16)


def draw_key_rows(key, part):
    return planted_pair(key)[1].astype(jnp.bfloat16)


def gain_of(base, salt):
    return 1.0 + 0.18 * jnp.clip(jax.random.normal(jax.random.fold_in(base, salt), (HEAD_DIM,), jnp.float32), -4.0, 4.0)


def draw_query_gain(key, part):
    return gain_of(key, 505).astype(jnp.bfloat16)


def draw_key_gain(key, part):
    return gain_of(key, 606).astype(jnp.bfloat16)


def draw_position_bias(key, part):
    table = 0.5 * jnp.clip(jax.random.normal(jax.random.fold_in(key, 808), (HEADS, CLIP + SEG), jnp.float32), -6.0, 6.0)
    return table.astype(jnp.bfloat16)


def shard_levels(rng, extent, shards, least, largest):
    def one(dim, shards_of):
        steps = jax.random.uniform(jax.random.fold_in(jax.random.fold_in(rng, 6), dim), (shards_of,), jnp.float32, least / len(shards), largest / len(shards))
        return jnp.repeat(jnp.exp(steps), extent[dim] // shards_of).reshape((-1,) + (1,) * (len(extent) - dim - 1))

    gain = one(*shards[0])
    for cut in shards[1:]:
        gain = gain * one(*cut)
    return gain


def gaussian(rng, extent, spread, bound, shards=(), held_as=jnp.bfloat16):
    drawn = spread * jax.random.normal(rng, extent, jnp.float32)
    if shards:
        drawn = drawn * shard_levels(rng, extent, shards, -0.22, 0.18)
    return jnp.clip(drawn, -bound, bound).astype(held_as)


def setup_inputs(seed: int = 0) -> dict:
    key_of = jax.random.split(jax.random.key(seed), 8)
    query_rows = draw_query_rows(jax.random.fold_in(key_of[7], 71), 0)
    key_rows = draw_key_rows(jax.random.fold_in(key_of[7], 71), 0)
    value_rows = gaussian(key_of[2], (SEQ, HEADS * HEAD_DIM), 1.0, 6.0, ((0, 256), (1, 4)))
    query_gain = draw_query_gain(jax.random.fold_in(key_of[7], 71), 0)
    key_gain = draw_key_gain(jax.random.fold_in(key_of[7], 71), 0)
    position_bias = draw_position_bias(jax.random.fold_in(key_of[7], 71), 0)
    output_grad = gaussian(key_of[6], (SEQ, HEADS * HEAD_DIM), 4.0, 24.0, ((0, 256), (1, 4)))
    return {"query_rows": query_rows, "key_rows": key_rows, "value_rows": value_rows, "query_gain": query_gain, "key_gain": key_gain, "position_bias": position_bias, "output_grad": output_grad}


NORM_EPS = 1e-06

def unit_rows(values):
    widened = values.astype(jnp.float32)
    scale_rows = lax.rsqrt(lax.optimization_barrier(jnp.mean(widened * widened, axis=-1, keepdims=True)) + NORM_EPS)
    return (widened * scale_rows, scale_rows)

def band_of(segments, seg_count):
    return jnp.concatenate([segments[offset:offset + seg_count] for offset in range(LEFT + 1)], axis=1)

def unband(banded, seg_count):
    summed = jnp.zeros((seg_count + LEFT, SEG) + banded.shape[2:], jnp.float32)
    for offset in range(LEFT + 1):
        summed = summed.at[offset:offset + seg_count].add(banded[:, offset * SEG:(offset + 1) * SEG])
    return summed

def layout(seg_count):
    band_pos = np.repeat(np.arange(LEFT + 1), SEG)
    key_pos = np.tile(np.arange(SEG), LEFT + 1)
    query_pos = np.arange(SEG)[:, None]
    distance = (LEFT - band_pos)[None, :] * SEG + query_pos - key_pos[None, :]
    bias_index = (np.minimum(distance, CLIP) + SEG - 1).astype(np.int32)
    visible = np.arange(seg_count)[:, None] - LEFT + band_pos[None, :] >= 0
    segs_block = TOK_DEV // SEG
    query_seg_index = np.arange(seg_count)[:, None]
    key_seg_index = query_seg_index - LEFT + band_pos[None, :]
    crossing = (query_seg_index // segs_block != key_seg_index // segs_block).astype(np.float32)
    return (bias_index, visible, crossing)

def split_unband(banded, crossing, seg_count):
    cross_mask = jnp.asarray(crossing)[:, :, None]
    own_part = unband(banded * (1.0 - cross_mask), seg_count)[LEFT:].reshape(SEQ, HEAD_DIM)
    cross_part = unband(banded * cross_mask, seg_count)[LEFT:].reshape(SEQ, HEAD_DIM)
    cross_low = lax.optimization_barrier(cross_part.astype(jnp.bfloat16)).astype(jnp.float32)
    return own_part + cross_low

def reference(query_rows, key_rows, value_rows, query_gain, key_gain, position_bias, output_grad):
    seg_count = SEQ // SEG
    bias_index, visible, crossing = layout(seg_count)
    score_scale = HEAD_DIM ** (-0.5)
    gain_query = query_gain.astype(jnp.float32)
    gain_key = key_gain.astype(jnp.float32)

    def by_head(matrix):
        return matrix.reshape(SEQ, HEADS, HEAD_DIM).transpose(1, 0, 2)

    def one_head(inputs):
        query_head, key_head, value_head, grad_head, bias_table = inputs
        query_hat, query_scale = unit_rows(query_head)
        key_hat, key_scale = unit_rows(key_head)
        query_unit = lax.optimization_barrier((query_hat * gain_query).astype(jnp.bfloat16))
        key_unit = lax.optimization_barrier((key_hat * gain_key).astype(jnp.bfloat16))
        padding = jnp.zeros((LEFT * SEG, HEAD_DIM), jnp.bfloat16)
        key_band = band_of(jnp.concatenate([padding, key_unit], 0).reshape(seg_count + LEFT, SEG, HEAD_DIM), seg_count).astype(jnp.float32)
        value_band = band_of(jnp.concatenate([padding, value_head], 0).reshape(seg_count + LEFT, SEG, HEAD_DIM), seg_count).astype(jnp.float32)
        query_seg = query_unit.reshape(seg_count, SEG, HEAD_DIM).astype(jnp.float32)
        grad_seg = grad_head.reshape(seg_count, SEG, HEAD_DIM).astype(jnp.float32)
        row_bias = bias_table.astype(jnp.float32)[bias_index]
        scores = jnp.einsum('cqd,ckd->cqk', query_seg, key_band) * score_scale + row_bias[None]
        scores = jnp.where(visible[:, None, :], scores, -jnp.inf)
        row_peak = lax.optimization_barrier(jnp.max(scores, axis=-1, keepdims=True))
        raised = jnp.exp(scores - row_peak)
        weights = raised / lax.optimization_barrier(jnp.sum(raised, axis=-1, keepdims=True))
        weights_low = lax.optimization_barrier(weights.astype(jnp.bfloat16)).astype(jnp.float32)
        d_weights = jnp.einsum('cqd,ckd->cqk', grad_seg, value_band)
        row_delta = lax.optimization_barrier(jnp.sum(weights * d_weights, axis=-1, keepdims=True))
        d_scores = weights * (d_weights - row_delta)
        d_low = lax.optimization_barrier(d_scores.astype(jnp.bfloat16)).astype(jnp.float32)
        dq_unit = (jnp.einsum('cqk,ckd->cqd', d_low, key_band) * score_scale).reshape(SEQ, HEAD_DIM)
        dk_unit = split_unband(jnp.einsum('cqk,cqd->ckd', d_low, query_seg) * score_scale, crossing, seg_count)
        value_grad = split_unband(jnp.einsum('cqk,cqd->ckd', weights_low, grad_seg), crossing, seg_count)
        bias_grad = jnp.zeros((CLIP + SEG,), jnp.float32).at[bias_index.ravel()].add(lax.optimization_barrier(jnp.sum(d_scores, axis=0)).ravel())
        dq_scaled = dq_unit * gain_query
        query_grad = query_scale * (dq_scaled - query_hat * lax.optimization_barrier(jnp.mean(dq_scaled * query_hat, axis=-1, keepdims=True)))
        dk_scaled = dk_unit * gain_key
        key_grad = key_scale * (dk_scaled - key_hat * lax.optimization_barrier(jnp.mean(dk_scaled * key_hat, axis=-1, keepdims=True)))
        return (query_grad.astype(jnp.bfloat16), key_grad.astype(jnp.bfloat16), value_grad.astype(jnp.bfloat16), bias_grad, lax.optimization_barrier(jnp.sum(dq_unit * query_hat, axis=0)), lax.optimization_barrier(jnp.sum(dk_unit * key_hat, axis=0)))
    results = lax.map(one_head, (by_head(query_rows), by_head(key_rows), by_head(value_rows), by_head(output_grad), position_bias))

    def to_rows(stacked):
        return stacked.transpose(1, 0, 2).reshape(SEQ, HEADS * HEAD_DIM)
    return (to_rows(results[0]), to_rows(results[1]), to_rows(results[2]), results[3], lax.optimization_barrier(jnp.sum(results[4], axis=0)), lax.optimization_barrier(jnp.sum(results[5], axis=0)))
```

```python
import functools

import jax
import jax.numpy as jnp
from jax import lax
from jax.experimental import pallas as pl
from jax.experimental.pallas import tpu as pltpu
from jax.sharding import Mesh
from jax.sharding import PartitionSpec as P


SEG = 64
LEFT = 8
HEAD = 64
LANES = 128
RSPAN = 320
REACH = LEFT * SEG
NORM_EPS = 1e-06
HIDDEN = -1e30
SP = ("sp_0", "sp_1", "sp_2")
F32 = jnp.float32
BF16 = jnp.bfloat16


def iota(shape, dim):
    return lax.broadcasted_iota(jnp.int32, shape, dim)


def dot(left, right, contract):
    return lax.dot_general(left, right, (contract, ((), ())), preferred_element_type=F32)


def half_means(values):
    same_half = (iota((2 * LANES, LANES), 0) % LANES) // HEAD == iota((2 * LANES, LANES), 1) // HEAD
    weights = jnp.where(same_half, 1.0 / HEAD, 0.0).astype(BF16)
    high = values.astype(BF16)
    low = (values - high.astype(F32)).astype(BF16)
    return dot(jnp.concatenate([high, low], axis=1), weights, ((1,), (0,)))


def normed(rows):
    widened = rows.astype(F32)
    scale = lax.rsqrt(half_means(widened * widened) + NORM_EPS)
    return widened * scale, scale


def by_head(rows):
    first = iota(rows.shape, 1) < HEAD
    zero = jnp.zeros_like(rows)
    return jnp.concatenate([jnp.where(first, rows, zero), jnp.where(first, zero, rows)], axis=0)


def fold(values, combine):
    return combine(values.reshape(-1, 8, values.shape[-1]), axis=0)


def toeplitz(row):
    top = pltpu.roll(jnp.broadcast_to(row, (8, LANES)), 0, 1, stride=1, stride_axis=0)
    return jnp.concatenate([top] + [pltpu.roll(top, 8 * i, 1) for i in range(1, 16)], axis=0)


def diagonal_sums(tile):
    rows = tile.shape[0]
    while rows > 8:
        rows //= 2
        tile = tile[:rows] + pltpu.roll(tile[rows:], LANES - rows, 1)
    for step in (4, 2, 1):
        tile = tile + pltpu.roll(pltpu.roll(tile, LANES - step, 1), 8 - step, 0)
    return tile[:1]


def main_kernel(
    first_ref, query_ref, key_ref, value_ref, grad_ref, prior_key_ref, prior_value_ref,
    query_gain_ref, key_gain_ref, table_ref,
    query_grad_ref, dk_ref, dv_ref, cross_ref, copies_ref,
    q_hat_ref, q_scale_ref, q_two_ref, g_two_ref, k_hat_ref, k_ref, k_t_ref, v_ref,
    bias_ref, s_ref, dp_ref, w_low_ref, d_low_ref, d_sum_ref, small_ref,
):
    tokens = query_ref.shape[0]
    steps = tokens // LANES
    wide = LANES * 5
    pair = pl.program_id(0)
    hidden_prior = first_ref[0]

    query_gain = query_gain_ref[...]
    key_gain = key_gain_ref[...]
    q_hat, q_scale = normed(query_ref[...])
    q_hat_ref[...] = q_hat
    q_scale_ref[...] = q_scale
    q_unit = (q_hat * query_gain).astype(BF16) * jnp.asarray(HEAD**-0.5, BF16)
    for m in range(steps):
        rows = slice(m * LANES, (m + 1) * LANES)
        q_two_ref[2 * m * LANES : 2 * (m + 1) * LANES] = by_head(q_unit[rows])
        g_two_ref[2 * m * LANES : 2 * (m + 1) * LANES] = by_head(grad_ref[rows])
    for part_ref, v_part_ref, start in ((prior_key_ref, prior_value_ref, 0), (key_ref, value_ref, REACH)):
        count = part_ref.shape[0]
        k_hat, _ = normed(part_ref[...])
        k_hat_ref[start : start + count] = k_hat
        k_unit = (k_hat * key_gain).astype(BF16)
        k_ref[start : start + count] = k_unit
        k_t_ref[:, start : start + count] = (k_unit * jnp.asarray(HEAD**-0.5, BF16)).T
        v_ref[start : start + count] = v_part_ref[...]

    square = (LANES, LANES)
    after = iota(square, 1) >= iota(square, 0)
    upper = iota(square, 0) < HEAD
    left = iota(square, 1) < HEAD
    for head in range(2):
        lanes = slice(head * LANES, (head + 1) * LANES)
        table = table_ref[0, head : head + 1]
        far = jnp.broadcast_to(table[:, :1], square)
        near = toeplitz(table[:, :LANES])
        middle = toeplitz(table[:, LANES : 2 * LANES])
        outer = toeplitz(table[:, 2 * LANES :])
        bias_ref[0:LANES, lanes] = jnp.where(upper & ~left, HIDDEN, far)
        bias_ref[LANES : 2 * LANES, lanes] = far
        bias_ref[2 * LANES : 3 * LANES, lanes] = jnp.where(after, far, outer)
        bias_ref[3 * LANES : 4 * LANES, lanes] = jnp.where(after, outer, middle)
        bias_ref[4 * LANES : 5 * LANES, lanes] = jnp.where(
            ~upper & left, HIDDEN, jnp.where(after, middle, near)
        )

    far_sum = jnp.zeros((8, 2 * LANES), F32)
    query_gain_sum = jnp.zeros((8, LANES), F32)
    key_gain_sum = jnp.zeros((8, LANES), F32)
    peaks = {}

    def score_block(m, b):
        if m >= steps:
            return
        at = m * LANES
        cols = slice(2 * at, 2 * (at + LANES))
        band = slice(at + b * LANES, at + (b + 1) * LANES)
        rows = slice(b * LANES, (b + 1) * LANES)
        scores = dot(k_ref[band], q_two_ref[cols], ((1,), (1,))) + bias_ref[rows]
        if m + b < 4:
            scores = scores + hidden_prior
        s_ref[m % 2, rows] = scores
        top = fold(scores, jnp.max)
        peaks[m] = top if b == 0 else jnp.maximum(peaks[m], top)
        dp_ref[m % 2, rows] = dot(v_ref[band], g_two_ref[cols], ((1,), (1,)))

    def query_side(m):
        at = m * LANES
        cols = slice(2 * at, 2 * (at + LANES))
        dq_t = dot(k_t_ref[:, at : at + wide], d_low_ref[at : at + wide, cols], ((1,), (0,)))
        dq = jnp.where(iota(square, 0) < HEAD, dq_t[:, :LANES], dq_t[:, LANES:]).T
        here = slice(at, at + LANES)
        q_hat = q_hat_ref[here]
        scaled = dq * query_gain
        mean = half_means(scaled * q_hat)
        query_grad_ref[here] = (q_scale_ref[here] * (scaled - q_hat * mean)).astype(BF16)
        return fold(dq * q_hat, jnp.sum)

    def key_side(j, low, high):
        band = slice(j * LANES, (j + 1) * LANES)
        cols = slice(2 * low * LANES, 2 * high * LANES)
        dk = dot(d_low_ref[band, cols], q_two_ref[cols], ((1,), (0,)))
        dv = dot(w_low_ref[band, cols], g_two_ref[cols], ((1,), (0,)))
        return dk, dv

    for b in range(5):
        score_block(0, b)
    for m in range(steps):
        at = m * LANES
        cols = slice(2 * at, 2 * (at + LANES))
        peak = jnp.max(peaks[m], axis=0, keepdims=True)
        total = jnp.zeros((8, 2 * LANES), F32)
        delta = jnp.zeros((8, 2 * LANES), F32)
        for b in range(5):
            rows = slice(b * LANES, (b + 1) * LANES)
            raised = jnp.exp(s_ref[m % 2, rows] - peak)
            s_ref[m % 2, rows] = raised
            total = total + fold(raised, jnp.sum)
            delta = delta + fold(raised * dp_ref[m % 2, rows], jnp.sum)
            score_block(m + 1, b)
        inverse = 1.0 / jnp.sum(total, axis=0, keepdims=True)
        delta = jnp.sum(delta, axis=0, keepdims=True) * inverse
        if m > 0:
            query_gain_sum = query_gain_sum + query_side(m - 1)
        for b in range(5):
            rows = slice(b * LANES, (b + 1) * LANES)
            band = slice(at + b * LANES, at + (b + 1) * LANES)
            weights = s_ref[m % 2, rows] * inverse
            d_scores = weights * (dp_ref[m % 2, rows] - delta)
            w_low_ref[band, cols] = weights.astype(BF16)
            d_low_ref[band, cols] = d_scores.astype(BF16)
            if b < 2:
                far_sum = far_sum + fold(d_scores, jnp.sum)
            else:
                kept = slice((b - 2) * LANES, (b - 1) * LANES)
                d_sum_ref[kept] = d_scores if m == 0 else d_sum_ref[kept] + d_scores
        if m < 4:
            dk, dv = key_side(m, 0, m + 1)
            band = slice(m * LANES, (m + 1) * LANES)
            dk_low = dk.astype(BF16)
            cross_ref[band] = dk_low
            cross_ref[REACH + m * LANES : REACH + (m + 1) * LANES] = dv.astype(BF16)
            key_gain_sum = key_gain_sum + fold(dk_low.astype(F32) * k_hat_ref[band], jnp.sum)
        if m == steps - 2:
            for j in range(4, steps + 3):
                dk_ref[(j - 4) * LANES : (j - 3) * LANES], dv_ref[(j - 4) * LANES : (j - 3) * LANES] = key_side(j, j - 4, m + 1)
    query_gain_sum = query_gain_sum + query_side(steps - 1)
    for j in range(4, steps + 4):
        here = slice((j - 4) * LANES, (j - 3) * LANES)
        dk, dv = key_side(j, steps - 1, steps)
        if j < steps + 3:
            dk = dk_ref[here] + dk
            dv = dv_ref[here] + dv
        dk_ref[here] = dk
        dv_ref[here] = dv
        key_gain_sum = key_gain_sum + fold(dk * k_hat_ref[j * LANES : (j + 1) * LANES], jnp.sum)

    tails = []
    for head in range(2):
        lanes = slice(head * LANES, (head + 1) * LANES)
        two, three, four = (d_sum_ref[i * LANES : (i + 1) * LANES, lanes] for i in range(3))
        zero = jnp.zeros(square, F32)
        far = far_sum[:, lanes] + fold(jnp.where(after, two, zero), jnp.sum)
        far = jnp.sum(jnp.sum(far, axis=0, keepdims=True), axis=1, keepdims=True)
        small_ref[pl.ds(5 * pair + 2 * head, 1)] = diagonal_sums(jnp.where(after, four, three))
        small_ref[pl.ds(5 * pair + 2 * head + 1, 1)] = diagonal_sums(jnp.where(after, three, two))
        tail = diagonal_sums(jnp.where(after, zero, four))
        tails.append(jnp.where(iota((1, LANES), 1) == HEAD, far, tail))
    first_half = iota((1, LANES), 1) < HEAD
    small_ref[pl.ds(5 * pair + 4, 1)] = jnp.where(first_half, pltpu.roll(tails[0], HEAD, 1), tails[1])
    both = []
    for part in (query_gain_sum, key_gain_sum):
        part = jnp.sum(part, axis=0, keepdims=True)
        both.append(part + pltpu.roll(part, HEAD, 1))
    gains = jnp.where(first_half, both[0], both[1])

    @pl.when(pair == 0)
    def _():
        small_ref[15:16] = gains

    @pl.when(pair > 0)
    def _():
        small_ref[15:16] = small_ref[15:16] + gains

    @pl.when(pair == pl.num_programs(0) - 1)
    def _():
        for copy in range(copies_ref.shape[0]):
            copies_ref[copy] = small_ref[...]


def final_kernel(key_ref, dk_ref, dv_ref, back_key_ref, back_value_ref, key_gain_ref, key_grad_ref, value_grad_ref):
    tokens = key_ref.shape[0]
    own = tokens - REACH
    for start, count in ((0, own), (own, REACH)):
        rows = slice(start, start + count)
        dk = dk_ref[rows]
        dv = dv_ref[rows]
        if start:
            dk = dk + back_key_ref[...].astype(F32)
            dv = dv + back_value_ref[...].astype(F32)
        value_grad_ref[rows] = dv.astype(BF16)
        k_hat, k_scale = normed(key_ref[rows])
        scaled = dk * key_gain_ref[...]
        mean = half_means(scaled * k_hat)
        key_grad_ref[rows] = (k_scale * (scaled - k_hat * mean)).astype(BF16)


def columns(rows, block=0):
    return pl.BlockSpec((rows, LANES), lambda p: (block, p))


def fixed(shape):
    return pl.BlockSpec(shape, lambda p: (0,) * len(shape))


def main_call(interpret, copies, first, query, key, value, grad, prior, query_gain, key_gain, table):
    tokens, width = query.shape
    pairs = width // LANES
    extended = tokens + REACH
    own = columns(tokens)
    placed = jax.ShapeDtypeStruct if interpret else pltpu.HBM
    return pl.pallas_call(
        main_kernel,
        grid=(pairs,),
        in_specs=[
            pl.BlockSpec(memory_space=pltpu.SMEM), own, own, own, own,
            columns(REACH), columns(REACH, 1), fixed((1, LANES)), fixed((1, LANES)),
            pl.BlockSpec((1, 2, 3 * LANES), lambda p: (p, 0, 0)),
        ],
        out_specs=[own, own, own, columns(2 * REACH), fixed((copies, 16, LANES))],
        out_shape=[
            placed((tokens, width), BF16),
            placed((tokens, width), F32),
            placed((tokens, width), F32),
            placed((2 * REACH, width), BF16),
            placed((copies, 16, LANES), F32),
        ],
        scratch_shapes=[
            pltpu.VMEM((tokens, LANES), F32),
            pltpu.VMEM((tokens, LANES), F32),
            pltpu.VMEM((2 * tokens, LANES), BF16),
            pltpu.VMEM((2 * tokens, LANES), BF16),
            pltpu.VMEM((extended, LANES), F32),
            pltpu.VMEM((extended, LANES), BF16),
            pltpu.VMEM((LANES, extended), BF16),
            pltpu.VMEM((extended, LANES), BF16),
            pltpu.VMEM((5 * LANES, 2 * LANES), F32),
            pltpu.VMEM((2, 5 * LANES, 2 * LANES), F32),
            pltpu.VMEM((2, 5 * LANES, 2 * LANES), F32),
            pltpu.VMEM((extended, 2 * tokens), BF16),
            pltpu.VMEM((extended, 2 * tokens), BF16),
            pltpu.VMEM((3 * LANES, 2 * LANES), F32),
            pltpu.VMEM((16, LANES), F32),
        ],
        compiler_params=None if interpret else pltpu.CompilerParams(vmem_limit_bytes=40 * 2**20),
        interpret=interpret,
        name="band_backward",
    )(first, query, key, value, grad, prior, prior, query_gain, key_gain, table)


def final_call(interpret, key, dk, dv, back, key_gain):
    tokens, width = key.shape
    own = columns(tokens)
    return pl.pallas_call(
        final_kernel,
        grid=(width // LANES,),
        in_specs=[own, own, own, columns(REACH), columns(REACH, 1), fixed((1, LANES))],
        out_specs=[own, own],
        out_shape=[jax.ShapeDtypeStruct((tokens, width), BF16)] * 2,
        interpret=interpret,
        name="key_and_value",
    )(key, dk, dv, back, back, key_gain)


def passed_along(block, axis, distance):
    devices = range(lax.axis_size(axis))
    route = [(i - distance, i) for i in devices if i - distance in devices]
    return lax.ppermute(block, axis, route)


def spread_sum(block, axes):
    return summed_copies(jnp.broadcast_to(block[None], (lax.axis_size(axes),) + block.shape), axes)


def summed_copies(copies, axes):
    return jnp.sum(lax.all_to_all(copies, axes, 0, 0), axis=0)


def body(query_rows, key_rows, value_rows, query_gain, key_gain, position_bias, output_grad, interpret=False):
    tokens = query_rows.shape[0]
    heads = position_bias.shape[0]
    pairs = heads // 2
    sent = jnp.concatenate([key_rows[tokens - REACH :], value_rows[tokens - REACH :]], axis=0)
    prior = passed_along(sent, SP, 1)
    gain_query = jnp.tile(query_gain.astype(F32), 2)[None]
    gain_key = jnp.tile(key_gain.astype(F32), 2)[None]
    table = position_bias.astype(F32)
    table = jnp.concatenate(
        [table[:, -1:], jnp.zeros((heads, 3 * LANES - RSPAN), F32), table[:, :-1]], axis=1
    ).reshape(pairs, 2, 3 * LANES)
    first = jnp.where(lax.axis_index(SP) == 0, HIDDEN, 0.0).astype(F32).reshape(1)
    query_grad, dk, dv, cross, copies = main_call(
        interpret, lax.axis_size("sp_0"), first, query_rows, key_rows, value_rows, output_grad, prior,
        gain_query, gain_key, table,
    )
    back = passed_along(cross, SP, -1)
    small = summed_copies(copies, "sp_0")
    small = spread_sum(small, ("sp_1", "sp_2"))
    gains = spread_sum(small[15:16], "tp")
    key_grad, value_grad = final_call(interpret, key_rows, dk, dv, back, gain_key)
    per_pair = small[:15].reshape(pairs, 5, LANES)
    tails = per_pair[:, 4].reshape(pairs, 2, HEAD)
    bias_grad = jnp.concatenate(
        [tails[:, :, 1:], per_pair[:, :4].reshape(pairs, 2, 2 * LANES), tails[:, :, :1]], axis=2
    ).reshape(heads, RSPAN)
    return query_grad, key_grad, value_grad, bias_grad, gains[0, :HEAD], gains[0, HEAD:]


def solution(mesh, sp_shape=(16, 8, 2), interpret=False):
    torus = Mesh(mesh.devices.reshape(*sp_shape, mesh.shape["tp"]), SP + ("tp",))
    placed = (P(SP, "tp"), P(SP, "tp"), P(SP, "tp"), P(), P(), P("tp", None), P(SP, "tp"))
    return jax.shard_map(
        functools.partial(body, interpret=interpret),
        mesh=torus,
        in_specs=placed,
        out_specs=(P(SP, "tp"), P(SP, "tp"), P(SP, "tp"), P("tp", None), P(), P()),
        check_vma=False,
    )
```

```python
import functools

import jax
import jax.numpy as jnp
from jax import lax
from jax.experimental import pallas as pl
from jax.experimental.pallas import tpu as pltpu
from jax.sharding import Mesh
from jax.sharding import PartitionSpec as P


SEG = 64
LEFT = 8
HEAD = 64
LANES = 128
RSPAN = 320
REACH = LEFT * SEG
NORM_EPS = 1e-06
HIDDEN = -1e30
LOCAL_MIB, MAIN_MIB, VALUE_MIB = 14, 18, 14
SP = ("sp_0", "sp_1", "sp_2")
F32 = jnp.float32
BF16 = jnp.bfloat16


def iota(shape, dim):
    return lax.broadcasted_iota(jnp.int32, shape, dim)


def dot(left, right, contract):
    return lax.dot_general(left, right, (contract, ((), ())), preferred_element_type=F32)


def half_means(values):
    same_half = (iota((2 * LANES, LANES), 0) % LANES) // HEAD == iota((2 * LANES, LANES), 1) // HEAD
    weights = jnp.where(same_half, 1.0 / HEAD, 0.0).astype(BF16)
    high = values.astype(BF16)
    low = (values - high.astype(F32)).astype(BF16)
    return dot(jnp.concatenate([high, low], axis=1), weights, ((1,), (0,)))


def normed(rows):
    widened = rows.astype(F32)
    scale = lax.rsqrt(half_means(widened * widened) + NORM_EPS)
    return widened * scale, scale


def by_head(rows):
    first = iota(rows.shape, 1) < HEAD
    zero = jnp.zeros_like(rows)
    return jnp.concatenate([jnp.where(first, rows, zero), jnp.where(first, zero, rows)], axis=0)


def fold(values, combine):
    return combine(values.reshape(-1, 8, values.shape[-1]), axis=0)


def toeplitz(row):
    top = pltpu.roll(jnp.broadcast_to(row, (8, LANES)), 0, 1, stride=1, stride_axis=0)
    return jnp.concatenate([top] + [pltpu.roll(top, 8 * i, 1) for i in range(1, 16)], axis=0)


def diagonal_sums(tile):
    rows = tile.shape[0]
    while rows > 8:
        rows //= 2
        tile = tile[:rows] + pltpu.roll(tile[rows:], LANES - rows, 1)
    for step in (4, 2, 1):
        tile = tile + pltpu.roll(pltpu.roll(tile, LANES - step, 1), 8 - step, 0)
    return tile[:1]


def norm_queries(rows, gain, hat_ref, scale_ref, two_ref):
    hat, scale = normed(rows)
    hat_ref[...] = hat
    scale_ref[...] = scale
    split_heads((hat * gain).astype(BF16) * jnp.asarray(HEAD**-0.5, BF16), two_ref)


def split_heads(rows, two_ref):
    for m in range(rows.shape[0] // LANES):
        two_ref[2 * m * LANES : 2 * (m + 1) * LANES] = by_head(rows[m * LANES : (m + 1) * LANES])


def norm_keys(rows, gain):
    hat, _ = normed(rows)
    unit = (hat * gain).astype(BF16)
    return hat, unit, (unit * jnp.asarray(HEAD**-0.5, BF16)).T


def write_bias(table_ref, bias_ref):
    square = (LANES, LANES)
    after = iota(square, 1) >= iota(square, 0)
    upper = iota(square, 0) < HEAD
    left = iota(square, 1) < HEAD
    for head in range(2):
        lanes = slice(head * LANES, (head + 1) * LANES)
        table = table_ref[0, head : head + 1]
        far = jnp.broadcast_to(table[:, :1], square)
        near = toeplitz(table[:, :LANES])
        middle = toeplitz(table[:, LANES : 2 * LANES])
        outer = toeplitz(table[:, 2 * LANES :])
        bias_ref[0:LANES, lanes] = jnp.where(upper & ~left, HIDDEN, far)
        bias_ref[LANES : 2 * LANES, lanes] = far
        bias_ref[2 * LANES : 3 * LANES, lanes] = jnp.where(after, far, outer)
        bias_ref[3 * LANES : 4 * LANES, lanes] = jnp.where(after, outer, middle)
        bias_ref[4 * LANES : 5 * LANES, lanes] = jnp.where(
            ~upper & left, HIDDEN, jnp.where(after, middle, near)
        )


def local_blocks():
    return [(m, b) for m in range(4) for b in range(4 - m, 5)]


def rows_at(index, size=LANES):
    return slice(index * size, (index + 1) * size)


def sweep(blocks, base, score_block, read_block, keep, far_sum, old_sum, between, following):
    s_ref, keep_weights, d_low_ref, d_sum_ref = keep
    peaks = {}

    def key_rows(j):
        return rows_at(j - base)

    def ahead(m, b):
        if m in blocks:
            top = score_block(m, b)
            if top is not None:
                peaks[m] = jnp.maximum(peaks[m], top) if m in peaks else top

    for b in range(5):
        ahead(blocks[0], b)
    for m in blocks:
        cols = rows_at(m - blocks[0], 2 * LANES)
        peak = jnp.max(peaks[m], axis=0, keepdims=True)
        total = jnp.zeros((8, 2 * LANES), F32)
        delta = jnp.zeros((8, 2 * LANES), F32)
        for b in range(5):
            scores, d_weights = read_block(m, b)
            raised = jnp.exp(scores - peak)
            s_ref[m % 2, rows_at(b)] = raised
            total = total + fold(raised, jnp.sum)
            delta = delta + fold(raised * d_weights, jnp.sum)
            ahead(m + 1, b)
        inverse = 1.0 / jnp.sum(total, axis=0, keepdims=True)
        delta = jnp.sum(delta, axis=0, keepdims=True) * inverse
        between(m)
        for b in range(5):
            weights = s_ref[m % 2, rows_at(b)] * inverse
            d_scores = weights * (read_block(m, b)[1] - delta)
            keep_weights(m, b, weights.astype(BF16))
            d_low_ref[key_rows(m + b), cols] = d_scores.astype(BF16)
            if b < 2:
                far_sum = far_sum + fold(d_scores, jnp.sum)
            else:
                kept_rows = rows_at(b - 2)
                if m > blocks[0]:
                    d_scores = d_sum_ref[kept_rows] + d_scores
                elif old_sum is not None:
                    d_scores = old_sum[kept_rows] + d_scores
                d_sum_ref[kept_rows] = d_scores
        following(m)
    return far_sum


def query_of(dq_t):
    return jnp.where(iota((LANES, LANES), 0) < HEAD, dq_t[:, :LANES], dq_t[:, LANES:]).T


def unnormed(grad, hat, scale, gain):
    scaled = grad * gain
    return (scale * (scaled - hat * half_means(scaled * hat))).astype(BF16)


def local_kernel(
    query_ref, key_ref, value_ref, grad_ref, query_gain_ref, key_gain_ref, table_ref,
    q_hat_out, q_two_out, g_two_out, k_hat_out, k_t_out, bias_out, d_sum_out, part_out,
    dk_out, s_out, dp_out, peak_out, q_scale_ref, dv_ref, query_grad_ref,
    k_ref, s_ref, dp_ref, w_low_ref, d_low_ref,
):
    last = query_ref.shape[0] // LANES - 1
    pair = pl.program_id(0)
    q_hat_ref, q_two_ref, g_two_ref, k_t_ref, bias_ref, s_local_ref, dp_local_ref = (
        ref.at[pair] for ref in (q_hat_out, q_two_out, g_two_out, k_t_out, bias_out, s_out, dp_out)
    )
    norm_queries(query_ref[...], query_gain_ref[...], q_hat_ref, q_scale_ref, q_two_ref)
    split_heads(grad_ref[...], g_two_ref)
    k_hat_out[pair], k_ref[...], k_t_ref[...] = norm_keys(key_ref[...], key_gain_ref[...])
    write_bias(table_ref, bias_ref)

    def products(m, b):
        keys = rows_at(m + b - 4)
        two = rows_at(m, 2 * LANES)
        scores = dot(k_ref[keys], q_two_ref[two], ((1,), (1,))) + bias_ref[rows_at(b)]
        return scores, dot(value_ref[keys], g_two_ref[two], ((1,), (1,)))

    def score_block(m, b):
        s_ref[m % 2, rows_at(b)], dp_ref[rows_at(b)] = scores, _ = products(m, b)
        return fold(scores, jnp.max)

    def keep_weights(m, b, weights):
        w_low_ref[rows_at(b)] = weights

    own = rows_at(last, 2 * LANES)
    far_sum = sweep(
        [last], 4, score_block, lambda m, b: (s_ref[m % 2, rows_at(b)], dp_ref[rows_at(b)]),
        (s_ref, keep_weights, d_low_ref, d_sum_out.at[pair]),
        jnp.zeros((8, 2 * LANES), F32), None, lambda m: None, lambda m: None,
    )
    here = rows_at(last)
    dq = query_of(dot(k_t_ref[...], d_low_ref[...], ((1,), (0,))))
    q_hat = q_hat_ref[here]
    query_grad_ref[...] = unnormed(dq, q_hat, q_scale_ref[here], query_gain_ref[...])
    part_out[pair, :, : 2 * LANES] = far_sum
    part_out[pair, :, 2 * LANES :] = fold(dq * q_hat, jnp.sum)
    dk_out[pair] = dot(d_low_ref[...], q_two_ref[own], ((1,), (0,)))
    dv_ref[...] = dot(w_low_ref[...], g_two_ref[own], ((1,), (0,)))
    peaks = {}
    for i, (m, b) in enumerate(local_blocks()):
        s_local_ref[rows_at(i)], dp_local_ref[rows_at(i)] = scores, _ = products(m, b)
        top = fold(scores, jnp.max)
        peaks[m] = jnp.maximum(peaks[m], top) if m in peaks else top
    for m, top in peaks.items():
        peak_out[pair, rows_at(m, 8)] = top


def main_kernel(
    first_ref, prior_ref, key_gain_ref,
    q_hat_in, q_two_in, g_two_in, k_hat_in, k_t_in, bias_in, d_sum_in, part_in, dk_in, s_in, dp_in, peak_in,
    dq_ref, w_low_ref, cross_ref, dk_ref, copies_ref,
    k_hat_prior, k_prior, k_t_prior, s_ref, dp_ref, d_low_ref, d_sum_ref, small_ref,
):
    count = dq_ref.shape[0] // LANES
    pair = pl.program_id(0)
    lanes_of_pair = pl.ds(pl.multiple_of(pair * LANES, LANES), LANES)
    q_hat_ref, q_two_ref, g_two_ref, own_hat_ref, bias_ref, s_local_ref, dp_local_ref = (
        ref.at[pair] for ref in (q_hat_in, q_two_in, g_two_in, k_hat_in, bias_in, s_in, dp_in)
    )
    index_of = {block: i for i, block in enumerate(local_blocks())}

    @pl.when(pair == 0)
    def _():
        for p in range(k_prior.shape[0]):
            k_hat_prior[p], k_prior[p], k_t_prior[p] = norm_keys(
                prior_ref[:REACH, p * LANES : (p + 1) * LANES], key_gain_ref[...]
            )

    k_ref, k_t_ref = k_prior.at[pair], k_t_prior.at[pair]
    gain_sums = [part_in[pair, :, 2 * LANES :], jnp.zeros((8, LANES), F32)]

    def score_block(m, b):
        if (m, b) in index_of:
            return peak_in[pair, rows_at(m, 8)] if b == 4 else None
        two = rows_at(m, 2 * LANES)
        scores = dot(k_ref[rows_at(m + b)], q_two_ref[two], ((1,), (1,))) + bias_ref[rows_at(b)] + first_ref[0]
        s_ref[m % 2, rows_at(b)] = scores
        values = prior_ref[REACH + (m + b) * LANES : REACH + (m + b + 1) * LANES, lanes_of_pair]
        dp_ref[m % 2, rows_at(b)] = dot(values, g_two_ref[two], ((1,), (1,)))
        return fold(scores, jnp.max)

    def read_block(m, b):
        if (m, b) in index_of:
            rows = rows_at(index_of[m, b])
            return s_local_ref[rows], dp_local_ref[rows]
        return s_ref[m % 2, rows_at(b)], dp_ref[m % 2, rows_at(b)]

    def keep_weights(m, b, weights):
        w_low_ref[rows_at(5 * m + b)] = weights

    def finish_query(m):
        if m < 0:
            return
        at = m * LANES
        cols = rows_at(m, 2 * LANES)
        dq_t = dot(k_t_ref[:, at:], d_low_ref[at:REACH, cols], ((1,), (0,)))
        dq_t = dq_t + dot(
            k_t_in[pair, :, : at + LANES], d_low_ref[REACH : REACH + at + LANES, cols], ((1,), (0,))
        )
        dq = query_of(dq_t)
        dq_ref[rows_at(m)] = dq
        gain_sums[0] = gain_sums[0] + fold(dq * q_hat_ref[rows_at(m)], jnp.sum)

    def key_side(j, low, high):
        cols = slice(2 * low * LANES, 2 * high * LANES)
        return dot(d_low_ref[rows_at(j), cols], q_two_ref[cols], ((1,), (0,)))

    def finish_keys(m):
        dk_low = key_side(m, 0, m + 1).astype(BF16)
        cross_ref[rows_at(m)] = dk_low
        gain_sums[1] = gain_sums[1] + fold(dk_low.astype(F32) * k_hat_prior[pair, rows_at(m)], jnp.sum)

    far_sum = sweep(
        list(range(count)), 0, score_block, read_block, (s_ref, keep_weights, d_low_ref, d_sum_ref),
        part_in[pair, :, : 2 * LANES], d_sum_in.at[pair], lambda m: finish_query(m - 1), finish_keys,
    )
    finish_query(count - 1)
    for j in range(4, count + 5):
        here = rows_at(j - 4)
        dk = dk_in[pair, here]
        if j < count + 4:
            dk = dk + key_side(j, j - 4, count)
        dk_ref[here] = dk
        gain_sums[1] = gain_sums[1] + fold(dk * own_hat_ref[here], jnp.sum)

    square = (LANES, LANES)
    after = iota(square, 1) >= iota(square, 0)
    tails = []
    for head in range(2):
        lanes = rows_at(head)
        two, three, four = (d_sum_ref[rows_at(i), lanes] for i in range(3))
        zero = jnp.zeros(square, F32)
        far = far_sum[:, lanes] + fold(jnp.where(after, two, zero), jnp.sum)
        far = jnp.sum(jnp.sum(far, axis=0, keepdims=True), axis=1, keepdims=True)
        small_ref[pl.ds(5 * pair + 2 * head, 1)] = diagonal_sums(jnp.where(after, four, three))
        small_ref[pl.ds(5 * pair + 2 * head + 1, 1)] = diagonal_sums(jnp.where(after, three, two))
        tail = diagonal_sums(jnp.where(after, zero, four))
        tails.append(jnp.where(iota((1, LANES), 1) == HEAD, far, tail))
    first_half = iota((1, LANES), 1) < HEAD
    small_ref[pl.ds(5 * pair + 4, 1)] = jnp.where(first_half, pltpu.roll(tails[0], HEAD, 1), tails[1])
    both = []
    for part in gain_sums:
        part = jnp.sum(part, axis=0, keepdims=True)
        both.append(part + pltpu.roll(part, HEAD, 1))
    gains = jnp.where(first_half, both[0], both[1])

    @pl.when(pair == 0)
    def _():
        small_ref[15:16] = gains

    @pl.when(pair > 0)
    def _():
        small_ref[15:16] = small_ref[15:16] + gains

    @pl.when(pair == pl.num_programs(0) - 1)
    def _():
        rows = copies_ref.shape[1]
        for copy in range(copies_ref.shape[0]):
            start = copy * rows % 16
            copies_ref[copy] = small_ref[start : start + rows]


def value_kernel(
    query_gain_ref, g_two_in, q_hat_in, w_low_ref, dv_ref, dq_ref, q_scale_ref, dk_cross_ref, last_grad_ref,
    query_grad_ref, dv_out, cross_ref,
):
    pair = pl.program_id(0)
    count = dq_ref.shape[0] // LANES
    cross_ref[:REACH] = dk_cross_ref[...]
    for j in range(count + 5):
        seen = range(max(0, j - 4), min(count, j + 1))
        if seen:
            weights = jnp.concatenate([w_low_ref[rows_at(4 * m + j)] for m in seen], axis=1)
            grads = g_two_in[pair, 2 * seen.start * LANES : 2 * seen.stop * LANES]
            dv = dot(weights, grads, ((1,), (0,)))
        if j < 4:
            cross_ref[rows_at(4 + j)] = dv.astype(BF16)
        else:
            own = dv_ref[rows_at(j - 4)]
            dv_out[rows_at(j - 4)] = own + dv if seen else own
    for m in range(count):
        here = rows_at(m)
        query_grad_ref[here] = unnormed(dq_ref[here], q_hat_in[pair, here], q_scale_ref[here], query_gain_ref[...])
    query_grad_ref[rows_at(count)] = last_grad_ref[...]


def final_kernel(key_ref, dk_ref, dv_ref, back_key_ref, back_value_ref, key_gain_ref, key_grad_ref, value_grad_ref):
    tokens = key_ref.shape[0]
    own = tokens - REACH
    for start, count in ((0, own), (own, REACH)):
        rows = slice(start, start + count)
        dk = dk_ref[rows]
        dv = dv_ref[rows]
        if start:
            dk = dk + back_key_ref[...].astype(F32)
            dv = dv + back_value_ref[...].astype(F32)
        value_grad_ref[rows] = dv.astype(BF16)
        k_hat, k_scale = normed(key_ref[rows])
        scaled = dk * key_gain_ref[...]
        mean = half_means(scaled * k_hat)
        key_grad_ref[rows] = (k_scale * (scaled - k_hat * mean)).astype(BF16)


def columns(rows, block=0):
    return pl.BlockSpec((rows, LANES), lambda p: (block, p))


def fixed(shape):
    return pl.BlockSpec(shape, lambda p: (0,) * len(shape))


def params(interpret, mebibytes):
    return None if interpret else pltpu.CompilerParams(vmem_limit_bytes=mebibytes * 2**20)


def in_vmem():
    return pl.BlockSpec(memory_space=pltpu.VMEM)


def local_call(interpret, query, key, value, grad, query_gain, key_gain, table):
    tokens, width = query.shape
    pairs = width // LANES
    own = columns(tokens)
    vmem = jax.ShapeDtypeStruct if interpret else pltpu.VMEM
    wide = 2 * LANES
    found = LANES * len(local_blocks())
    shapes = {
        "q_hat": ((tokens, LANES), F32),
        "q_two": ((2 * tokens, LANES), BF16),
        "g_two": ((2 * tokens, LANES), BF16),
        "k_hat": ((tokens, LANES), F32),
        "k_t": ((LANES, tokens), BF16),
        "bias": ((5 * LANES, wide), F32),
        "d_sum": ((3 * LANES, wide), F32),
        "part": ((8, 3 * LANES), F32),
        "dk": ((tokens, LANES), F32),
        "scores": ((found, wide), F32),
        "d_weights": ((found, wide), F32),
        "peaks": ((4 * 8, wide), F32),
    }
    hbm = jax.ShapeDtypeStruct if interpret else pltpu.HBM
    *arrays, q_scale, dv, last_grad = pl.pallas_call(
        local_kernel,
        grid=(pairs,),
        in_specs=[
            own, own, own, own, fixed((1, LANES)), fixed((1, LANES)),
            pl.BlockSpec((1, 2, 3 * LANES), lambda p: (p, 0, 0)),
        ],
        out_specs=[in_vmem()] * len(shapes) + [own, own, columns(LANES)],
        out_shape=[vmem((pairs,) + shape, dtype) for shape, dtype in shapes.values()]
        + [hbm((tokens, width), F32), hbm((tokens, width), F32), hbm((LANES, width), BF16)],
        scratch_shapes=[
            pltpu.VMEM((tokens, LANES), BF16),
            pltpu.VMEM((2, 5 * LANES, wide), F32),
            pltpu.VMEM((5 * LANES, wide), F32),
            pltpu.VMEM((5 * LANES, wide), BF16),
            pltpu.VMEM((5 * LANES, wide), BF16),
        ],
        compiler_params=params(interpret, LOCAL_MIB),
        interpret=interpret,
        name="local_backward",
    )(query, key, value, grad, query_gain, key_gain, table)
    return dict(zip(shapes, arrays)), (dv, q_scale, last_grad)


def weights_block(early):
    return pl.BlockSpec((None, 5 * early, 2 * LANES), lambda p: (p, 0, 0))


def main_call(interpret, far, halves, first, prior, key_gain, local):
    pairs, tokens = local["q_hat"].shape[:2]
    width = pairs * LANES
    extended = tokens + REACH
    early = tokens - LANES
    wide = 2 * LANES
    hbm = jax.ShapeDtypeStruct if interpret else pltpu.HBM
    copies = (far * halves, 16 // halves, LANES)
    taken = (
        "q_hat", "q_two", "g_two", "k_hat", "k_t", "bias", "d_sum", "part", "dk", "scores", "d_weights", "peaks",
    )
    return pl.pallas_call(
        main_kernel,
        grid=(pairs,),
        in_specs=[pl.BlockSpec(memory_space=pltpu.SMEM), in_vmem(), fixed((1, LANES))] + [in_vmem()] * len(taken),
        out_specs=[
            columns(early), weights_block(early), columns(REACH), columns(tokens), fixed(copies),
        ],
        out_shape=[
            hbm((early, width), F32),
            hbm((pairs, 5 * early, wide), BF16),
            hbm((REACH, width), BF16),
            hbm((tokens, width), F32),
            hbm(copies, F32),
        ],
        scratch_shapes=[
            pltpu.VMEM((pairs, REACH, LANES), F32),
            pltpu.VMEM((pairs, REACH, LANES), BF16),
            pltpu.VMEM((pairs, LANES, REACH), BF16),
            pltpu.VMEM((2, 5 * LANES, wide), F32),
            pltpu.VMEM((2, 5 * LANES, wide), F32),
            pltpu.VMEM((extended, 2 * early), BF16),
            pltpu.VMEM((3 * LANES, wide), F32),
            pltpu.VMEM((16, LANES), F32),
        ],
        compiler_params=params(interpret, MAIN_MIB),
        interpret=interpret,
        name="band_backward",
    )(first, prior, key_gain, *(local[name] for name in taken))


def value_call(interpret, query_gain, local, w_low, dv, dq, q_scale, dk_cross, last_grad):
    tokens, width = dv.shape
    early = dq.shape[0]
    hbm = jax.ShapeDtypeStruct if interpret else pltpu.HBM
    own = columns(tokens)
    return pl.pallas_call(
        value_kernel,
        grid=(width // LANES,),
        in_specs=[
            fixed((1, LANES)), in_vmem(), in_vmem(),
            weights_block(early), own, columns(early), own, columns(REACH), columns(LANES),
        ],
        out_specs=[own, own, columns(2 * REACH)],
        out_shape=[
            hbm((tokens, width), BF16),
            hbm((tokens, width), F32),
            hbm((2 * REACH, width), BF16),
        ],
        compiler_params=params(interpret, VALUE_MIB),
        interpret=interpret,
        name="value_backward",
    )(query_gain, local["g_two"], local["q_hat"], w_low, dv, dq, q_scale, dk_cross, last_grad)


def final_call(interpret, key, dk, dv, back, key_gain):
    tokens, width = key.shape
    own = columns(tokens)
    return pl.pallas_call(
        final_kernel,
        grid=(width // LANES,),
        in_specs=[own, own, own, columns(REACH), columns(REACH, 1), fixed((1, LANES))],
        out_specs=[own, own],
        out_shape=[jax.ShapeDtypeStruct((tokens, width), BF16)] * 2,
        interpret=interpret,
        name="key_and_value",
    )(key, dk, dv, back, back, key_gain)


def passed_along(block, axis, distance):
    devices = range(lax.axis_size(axis))
    route = [(i - distance, i) for i in devices if i - distance in devices]
    return lax.ppermute(block, axis, route)


def body(query_rows, key_rows, value_rows, query_gain, key_gain, position_bias, output_grad, interpret=False):
    tokens = query_rows.shape[0]
    heads = position_bias.shape[0]
    pairs = heads // 2
    gain_query = jnp.tile(query_gain.astype(F32), 2)[None]
    gain_key = jnp.tile(key_gain.astype(F32), 2)[None]
    table = position_bias.astype(F32)
    table = jnp.concatenate(
        [table[:, -1:], jnp.zeros((heads, 3 * LANES - RSPAN), F32), table[:, :-1]], axis=1
    ).reshape(pairs, 2, 3 * LANES)
    far, near, halves = (lax.axis_size(axis) for axis in SP)
    groups = lax.axis_size("tp")
    first = jnp.where(lax.axis_index(SP) == 0, HIDDEN, 0.0).astype(F32).reshape(1)
    sent = jnp.concatenate([key_rows[tokens - REACH :], value_rows[tokens - REACH :]], axis=0)
    prior = passed_along(sent, SP, 1)
    local, (dv, q_scale, last_grad) = local_call(
        interpret, query_rows, key_rows, value_rows, output_grad, gain_query, gain_key, table
    )
    dq, w_low, dk_cross, dk, copies = main_call(interpret, far, halves, first, prior, gain_key, local)
    query_grad, dv, cross = value_call(interpret, gain_query, local, w_low, dv, dq, q_scale, dk_cross, last_grad)
    back = passed_along(cross, SP, -1)
    half = jnp.sum(lax.all_to_all(copies, ("sp_0", "sp_2"), 0, 0), axis=0)
    spread = jnp.broadcast_to(half[None], (near * halves * groups,) + half.shape)
    spread = lax.all_to_all(spread, ("sp_1", "sp_2", "tp"), 0, 0)
    spread = jnp.sum(spread.reshape((near, halves, groups) + half.shape), axis=0)
    key_grad, value_grad = final_call(interpret, key_rows, dk, dv, back, gain_key)
    gains = jnp.sum(spread[-1, :, -1], axis=0)
    small = lax.dynamic_index_in_dim(spread, lax.axis_index("tp"), 1, keepdims=False).reshape(16, LANES)
    per_pair = small[:15].reshape(pairs, 5, LANES)
    tails = per_pair[:, 4].reshape(pairs, 2, HEAD)
    bias_grad = jnp.concatenate(
        [tails[:, :, 1:], per_pair[:, :4].reshape(pairs, 2, 2 * LANES), tails[:, :, :1]], axis=2
    ).reshape(heads, RSPAN)
    return query_grad, key_grad, value_grad, bias_grad, gains[:HEAD], gains[HEAD:]


def solution(mesh, sp_shape=(16, 8, 2), interpret=False):
    torus = Mesh(mesh.devices.reshape(*sp_shape, mesh.shape["tp"]), SP + ("tp",))
    placed = (P(SP, "tp"), P(SP, "tp"), P(SP, "tp"), P(), P(), P("tp", None), P(SP, "tp"))
    return jax.shard_map(
        functools.partial(body, interpret=interpret),
        mesh=torus,
        in_specs=placed,
        out_specs=(P(SP, "tp"), P(SP, "tp"), P(SP, "tp"), P("tp", None), P(), P()),
        check_vma=False,
    )
```
